32 devices in a mesh: ep: 4 (over y, x), tp: 8 (over z, core).
Axes of the slice: x: 2, y: 2, z: 4, core: 2. Of those that a mesh axis runs over, the one named last changes fastest.
Arguments:
- tokens: bfloat16 [64, 2048], P('ep'), may hold values from -6 to 6
- routes: int32 [64, 4], P('ep'), may hold values from 0 to 7, all different within a row; in each aligned block of 16 rows (0 to 15, 16 to 31, ...) at most 16 rows name the same one
- route_weight: float32 [64, 4], P('ep'), may hold values from 0.2 to 1
- mixer_gain: float32 [2048], replicated, may hold values from 0.1 to 1.9
- gate_weight: bfloat16 [2048, 4096], P(None, 'tp'), may hold values from -0.125 to 0.125
- input_weight: bfloat16 [2048, 4096], P(None, 'tp'), may hold values from -0.125 to 0.125
- step_weight: bfloat16 [2048, 64], P(None, 'tp'), may hold values from -0.125 to 0.125
- write_weight: bfloat16 [2048, 512], P('tp'), may hold values from -0.125 to 0.125
- read_weight: bfloat16 [2048, 512], P('tp'), may hold values from -0.125 to 0.125
- step_bias: float32 [64], P('tp'), may hold values from -3 to 0.5
- decay_log: float32 [64], P('tp'), may hold values from -2 to 0.5
- decay_jolt: float32 [64, 64], P('ep', 'tp'), may hold values from -1 to 0
- filter_taps: bfloat16 [4, 4096], P(None, 'tp'), may hold values from -3 to 3
- filter_state: bfloat16 [64, 3, 4096], P('ep', None, 'tp'), may hold values from -6 to 6
- scan_state: float32 [64, 64, 64, 128], P('ep', 'tp'), may hold values from -2 to 2
- skip_gain: float32 [64], P('tp'), may hold values from 0.5 to 2
- head_gain: float32 [4096], P('tp'), may hold values from 0.1 to 1.9
- output_weight: bfloat16 [4096, 2048], P('tp'), may hold values from -0.09375 to 0.09375
- channel_gain: float32 [2048], replicated, may hold values from 0.1 to 1.9
- expert_gate: bfloat16 [8, 2048, 2048], P('ep', None, 'tp'), may hold values from -0.125 to 0.125
- expert_up: bfloat16 [8, 2048, 2048], P('ep', None, 'tp'), may hold values from -0.125 to 0.125
- expert_down: bfloat16 [8, 2048, 2048], P('ep', 'tp'), may hold values from -0.125 to 0.125
- shared_gate: bfloat16 [2048, 2048], P(None, 'tp'), may hold values from -0.125 to 0.125
- shared_up: bfloat16 [2048, 2048], P(None, 'tp'), may hold values from -0.125 to 0.125
- shared_down: bfloat16 [2048, 2048], P('tp'), may hold values from -0.125 to 0.125
Outputs:
- layer_out: bfloat16 [64, 2048], P('ep', 'tp')
- new_state: float32 [64, 64, 64, 128], P('ep', 'tp')
- new_filter: bfloat16 [64, 3, 4096], P('ep', None, 'tp')
The draws below stay inside these ranges and needn't reach their ends.
Inputs may be any that keep to these rules, and one draw needn't show every extreme that they name: `routes`: each row names 4 different experts. In each aligned block of 16 rows (the rows of one index of ep) no expert is named by more than 16 rows, a bound that some block reaches.
All inputs are finite; a program needn't handle non-finite values.
Results may differ from the reference program's by a relative error of at most 0.025.
Values may be sent and summed in bfloat16 or wider, within the bound.
A program may use at most 64 MiB of HBM per device.

```python
import math
import jax
import jax.numpy as jnp
import numpy as np
from jax import lax

D = 2048
HEADS = 64
HEAD_DIM = 64
DI = 4096
GROUPS = 4
STATE = 128
CONV = 4
FF_E = 2048
FF_S = 2048
TOPK = 4
SEQ_DEV = 16
SEQS = 64
EXPERTS = 8
CAP = 16
N_EP = 4
N_TP = 8


def levels(own_key, dims, split, low, largest):
    gain = 1.0
    for dim, blocks in split:
        steps = jax.random.uniform(jax.random.fold_in(jax.random.fold_in(own_key, 6), dim), (blocks,), jnp.float32, low / len(split), largest / len(split))
        gain = gain * jnp.repeat(jnp.exp(steps), dims[dim] // blocks).reshape((-1,) + (1,) * (len(dims) - 1 - dim))
    return gain


def routed_block(stream_key, own, number, rows, count, top, reach, slope):
    ranking = jax.random.permutation(stream_key, count)
    crowded, ordinary = portions_of(count, rows * top, reach, slope, True), portions_of(count, rows * top, reach, slope, False)
    places = jnp.arange(count)

    def named(tallies, offset_by):
        used = int((tallies > 0).sum())
        fixed = max(1, used // 4)
        moved = fixed + (places - fixed + offset_by * (used - fixed)) % max(1, count - fixed)
        return jnp.zeros((count,), jnp.int32).at[ranking[jnp.where(places < fixed, places, moved)]].set(jnp.asarray(tallies, jnp.int32))

    tallies = jnp.where(number % 4 == 0, named(crowded, number // 4), named(ordinary, number - number // 4 - 1))
    mixed = jax.random.permutation(jax.random.fold_in(own, 3), count)
    donor, taker = mixed[0:count // 2 * 2:2], mixed[1:count // 2 * 2:2]
    margin = jnp.minimum(tallies[donor] - 1, reach - tallies[taker]) // 2
    margin = jnp.where((donor == ranking[0]) | (taker == ranking[0]) | (tallies[taker] == 0), 0, jnp.maximum(margin, 0))
    moved = jax.random.randint(jax.random.fold_in(own, 4), (count // 2,), 0, 1 << 20) % (margin + 1)
    tallies = tallies.at[donor].add(-moved).at[taker].add(moved)
    items = jnp.searchsorted(jnp.cumsum(tallies), jnp.arange(rows * top), side="right").astype(jnp.int32)
    grid = items.reshape(top, rows).T
    grid = grid[jax.random.permutation(jax.random.fold_in(own, 1), rows)]
    offset_by = jax.random.randint(jax.random.fold_in(own, 2), (rows, 1), 0, top)
    return jnp.take_along_axis(grid, (jnp.arange(top)[None, :] + offset_by) % top, axis=1)


def portions_of(amount, total, limit, skew, full):
    loads = [(1 << 20) // math.isqrt(grade ** skew) + 1 for grade in range(1, amount + 1)]
    largest = limit if full else min(limit, max(-(-total // amount), total * loads[0] // sum(loads)))
    least = 1 if total - largest >= amount - 1 else 0
    counts, spare = [largest] + [least] * (amount - 1), total - largest - least * (amount - 1)
    while spare > 0:
        movable = [i for i in range(1, amount) if counts[i] < largest] or [i for i in range(1, amount) if counts[i] < limit]
        mass, left = sum([loads[i] for i in movable]), spare
        for i in movable:
            more = min(limit - counts[i], max(1, left * loads[i] // mass), spare)
            counts[i] = counts[i] + more
            spare = spare - more
    return np.array(counts)


def bell_draw(stream_key, extent, scale, reach, shards=(), kind=jnp.bfloat16):
    level = levels(stream_key, extent, shards, -0.22, 0.18) if shards else 1.0
    drawn = jax.random.normal(stream_key, extent, jnp.float32) * scale * level
    return jnp.minimum(jnp.maximum(drawn, -reach), reach).astype(kind)


def setup_inputs(seed: int = 0) -> dict:
    arg_keys = jax.random.split(jax.random.key(seed), 26)
    tokens = bell_draw(arg_keys[0], (SEQS, D), 1.0, 6.0, ((0, 4),))
    routes_keys = jax.random.split(jax.random.fold_in(arg_keys[1], 1), SEQS // SEQ_DEV)
    routes_turns = jax.random.permutation(jax.random.fold_in(arg_keys[1], 3), SEQS // SEQ_DEV)
    routes = jax.vmap(lambda own, number: routed_block(jax.random.fold_in(arg_keys[1], 2), own, number, SEQ_DEV, EXPERTS, TOPK, CAP, 2))(routes_keys, routes_turns).reshape((SEQS, TOPK))
    route_weight = jnp.clip(jnp.exp(math.log(1.0) - 1.609438 * jax.random.uniform(arg_keys[2], (SEQS, TOPK), jnp.float32) ** levels(arg_keys[2], (SEQS, TOPK), ((0, 4),), -0.2, 0.2)), 0.2, 1.0)
    mixer_gain = jnp.clip(1.0 + 0.18 * jax.random.normal(arg_keys[3], (D,), jnp.float32), 0.1, 1.9)
    gate_weight = bell_draw(arg_keys[4], (D, DI), D ** -0.5, 0.125, ((1, 8),))
    input_weight = bell_draw(arg_keys[5], (D, DI), D ** -0.5, 0.125, ((1, 8),))
    step_weight = bell_draw(arg_keys[6], (D, HEADS), D ** -0.5, 0.125, ((1, 8),))
    write_weight = bell_draw(arg_keys[7], (D, GROUPS * STATE), D ** -0.5, 0.125, ((0, 8),))
    read_weight = bell_draw(arg_keys[8], (D, GROUPS * STATE), D ** -0.5, 0.125, ((0, 8),))
    step_bias = jnp.clip(-3.0 + 3.5 * jax.random.uniform(arg_keys[9], (HEADS,), jnp.float32) ** levels(arg_keys[9], (HEADS,), ((0, 8),), -0.2, 0.2), -3.0, 0.5)
    decay_log = jnp.clip(-2.0 + 2.5 * jax.random.uniform(arg_keys[10], (HEADS,), jnp.float32) ** levels(arg_keys[10], (HEADS,), ((0, 8),), -0.2, 0.2), -2.0, 0.5)
    decay_jolt = jnp.clip(-1.0 + 1.0 * jax.random.uniform(arg_keys[11], (SEQS, HEADS), jnp.float32) ** levels(arg_keys[11], (SEQS, HEADS), ((0, 4), (1, 8)), -0.2, 0.2), -1.0, 0.0)
    filter_taps = bell_draw(arg_keys[12], (CONV, DI), 0.5, 3.0, ((1, 8),))
    filter_state = bell_draw(arg_keys[13], (SEQS, CONV - 1, DI), 1.0, 6.0, ((0, 4), (2, 8)))
    scan_state = bell_draw(arg_keys[14], (SEQS, HEADS, HEAD_DIM, STATE), 0.3, 2.0, ((0, 4), (1, 8)), jnp.float32)
    skip_gain = jnp.clip(jnp.exp(math.log(2.0) - 1.3862944 * jax.random.uniform(arg_keys[15], (HEADS,), jnp.float32) ** levels(arg_keys[15], (HEADS,), ((0, 8),), -0.2, 0.2)), 0.5, 2.0)
    head_gain = jnp.clip(1.0 + 0.18 * jax.random.normal(arg_keys[16], (DI,), jnp.float32), 0.1, 1.9)
    output_weight = bell_draw(arg_keys[17], (DI, D), DI ** -0.5, 0.09375, ((0, 8),))
    channel_gain = jnp.clip(1.0 + 0.18 * jax.random.normal(arg_keys[18], (D,), jnp.float32), 0.1, 1.9)
    expert_gate = bell_draw(arg_keys[19], (EXPERTS, D, FF_E), D ** -0.5, 0.125, ((0, 4), (2, 8)))
    expert_up = bell_draw(arg_keys[20], (EXPERTS, D, FF_E), D ** -0.5, 0.125, ((0, 4), (2, 8)))
    expert_down = bell_draw(arg_keys[21], (EXPERTS, FF_E, D), FF_E ** -0.5, 0.125, ((0, 4), (1, 8)))
    shared_gate = bell_draw(arg_keys[22], (D, FF_S), D ** -0.5, 0.125, ((1, 8),))
    shared_up = bell_draw(arg_keys[23], (D, FF_S), D ** -0.5, 0.125, ((1, 8),))
    shared_down = bell_draw(arg_keys[24], (FF_S, D), FF_S ** -0.5, 0.125, ((0, 8),))
    return {"tokens": tokens, "routes": routes, "route_weight": route_weight, "mixer_gain": mixer_gain, "gate_weight": gate_weight, "input_weight": input_weight, "step_weight": step_weight, "write_weight": write_weight, "read_weight": read_weight, "step_bias": step_bias, "decay_log": decay_log, "decay_jolt": decay_jolt, "filter_taps": filter_taps, "filter_state": filter_state, "scan_state": scan_state, "skip_gain": skip_gain, "head_gain": head_gain, "output_weight": output_weight, "channel_gain": channel_gain, "expert_gate": expert_gate, "expert_up": expert_up, "expert_down": expert_down, "shared_gate": shared_gate, "shared_up": shared_up, "shared_down": shared_down}


EPS = 1e-06

def rms_normed(values, scaling):
    mean_square = lax.optimization_barrier(jnp.mean(values * values, axis=-1, keepdims=True))
    return values * lax.rsqrt(mean_square + EPS) * scaling

def route_targets(route_ids, experts, capacity):
    count_rows, top_picks = route_ids.shape
    flattened = route_ids.reshape(count_rows * top_picks).astype(jnp.int32)
    onehot = (flattened[:, None] == jnp.arange(experts, dtype=jnp.int32)[None, :]).astype(jnp.int32)
    before = jnp.cumsum(onehot, axis=0) - onehot
    slot_index = lax.optimization_barrier(jnp.sum(before * onehot, axis=1))
    return (flattened * capacity + slot_index).astype(jnp.int32).reshape(count_rows, top_picks)

def shard_rounded(hidden, weight):
    count_rows = hidden.shape[0]
    slice_width = hidden.shape[1] // N_TP
    hidden_parts = hidden.reshape(count_rows, N_TP, slice_width).astype(jnp.float32)
    weight_parts = weight.reshape(N_TP, slice_width, weight.shape[1]).astype(jnp.float32)
    partial_sums = jnp.einsum('rtf,tfd->rtd', hidden_parts, weight_parts).astype(jnp.bfloat16)
    partial_sums = lax.optimization_barrier(partial_sums)
    return lax.optimization_barrier(jnp.sum(partial_sums.astype(jnp.float32), axis=1))

def reference(tokens, routes, route_weight, mixer_gain, gate_weight, input_weight, step_weight, write_weight, read_weight, step_bias, decay_log, decay_jolt, filter_taps, filter_state, scan_state, skip_gain, head_gain, output_weight, channel_gain, expert_gate, expert_up, expert_down, shared_gate, shared_up, shared_down):
    tokens_f = tokens.astype(jnp.float32)
    normed = rms_normed(tokens_f, mixer_gain).astype(jnp.bfloat16)
    write_in = jnp.dot(normed, write_weight, preferred_element_type=jnp.float32)
    read_in = jnp.dot(normed, read_weight, preferred_element_type=jnp.float32)
    gate_rows = jnp.dot(normed, gate_weight, preferred_element_type=jnp.float32).astype(jnp.bfloat16)
    input_rows = jnp.dot(normed, input_weight, preferred_element_type=jnp.float32).astype(jnp.bfloat16)
    step_raw = jnp.dot(normed, step_weight, preferred_element_type=jnp.float32)
    seq_count = tokens.shape[0]
    per_group = HEADS // GROUPS
    write_vec = jnp.repeat(jax.nn.silu(write_in).reshape(seq_count, GROUPS, STATE), per_group, axis=1)
    read_vec = jnp.repeat(jax.nn.silu(read_in).reshape(seq_count, GROUPS, STATE), per_group, axis=1)
    window = jnp.concatenate([filter_state, input_rows[:, None, :]], axis=1)
    filtered = jax.nn.silu(lax.optimization_barrier(jnp.sum(window.astype(jnp.float32) * filter_taps.astype(jnp.float32)[None], axis=1)))
    step_size = jax.nn.softplus(step_raw + step_bias)
    log_decay = decay_jolt - jnp.exp(decay_log) * step_size
    head_input = filtered.reshape(seq_count, HEADS, HEAD_DIM)
    new_state = jnp.exp(log_decay)[:, :, None, None] * scan_state + (step_size[:, :, None] * head_input)[:, :, :, None] * write_vec[:, :, None, :]
    readout = jnp.einsum('shpn,shn->shp', new_state, read_vec, precision=lax.Precision.HIGHEST)
    readout = readout + skip_gain[None, :, None] * head_input
    gate_heads = gate_rows.astype(jnp.float32).reshape(seq_count, HEADS, HEAD_DIM)
    gated = rms_normed(readout * jax.nn.silu(gate_heads), head_gain.reshape(HEADS, HEAD_DIM))
    gated = gated.astype(jnp.bfloat16).reshape(seq_count, HEADS * HEAD_DIM)
    mixed = jnp.dot(gated, output_weight, preferred_element_type=jnp.float32).astype(jnp.bfloat16)
    resid = (tokens_f + mixed.astype(jnp.float32)).astype(jnp.bfloat16)
    normed_ffn = rms_normed(resid.astype(jnp.float32), channel_gain).astype(jnp.bfloat16)
    shared_hidden = (jax.nn.silu(jnp.dot(normed_ffn, shared_gate, preferred_element_type=jnp.float32)) * jnp.dot(normed_ffn, shared_up, preferred_element_type=jnp.float32)).astype(jnp.bfloat16)
    shared_out = shard_rounded(shared_hidden, shared_down)
    targets = jax.vmap(lambda block: route_targets(block, EXPERTS, CAP))(routes.reshape(N_EP, SEQ_DEV, TOPK))
    block_index = jnp.arange(N_EP, dtype=jnp.int32)[:, None, None]
    expert_index = targets // CAP
    slot_index = targets % CAP
    position = ((expert_index * N_EP + block_index) * CAP + slot_index).reshape(-1).astype(jnp.int32)
    token_index = jnp.broadcast_to(jnp.arange(seq_count, dtype=jnp.int32).reshape(N_EP, SEQ_DEV, 1), targets.shape).reshape(-1)
    row_token = jnp.full((EXPERTS * N_EP * CAP,), seq_count, jnp.int32).at[position].set(token_index)
    padded = jnp.concatenate([normed_ffn, jnp.zeros((1, D), jnp.bfloat16)], axis=0)

    def one_expert(operands):
        token_ids, gate_part, up_part, down_part = operands
        chosen = padded[token_ids]
        hidden = (jax.nn.silu(jnp.dot(chosen, gate_part, preferred_element_type=jnp.float32)) * jnp.dot(chosen, up_part, preferred_element_type=jnp.float32)).astype(jnp.bfloat16)
        return shard_rounded(hidden, down_part).astype(jnp.bfloat16)
    expert_out = lax.map(one_expert, (row_token.reshape(EXPERTS, N_EP * CAP), expert_gate, expert_up, expert_down))
    picked = expert_out.reshape(EXPERTS * N_EP * CAP, D)[position].reshape(seq_count, TOPK, D)
    routed = lax.optimization_barrier(jnp.sum(route_weight[:, :, None] * picked.astype(jnp.float32), axis=1))
    layer_out = (resid.astype(jnp.float32) + shared_out + routed).astype(jnp.bfloat16)
    return (layer_out, new_state, window[:, 1:, :])
```

```python
import functools

import jax
import jax.numpy as jnp
from jax import lax
from jax.experimental import pallas as pl
from jax.experimental.pallas import tpu as pltpu
from jax.sharding import PartitionSpec as P

HEADS = 64
HEAD_DIM = 64
GROUPS = 4
STATE = 128

EPS = 1e-06
F32 = jnp.float32
BF16 = jnp.bfloat16
MESH = pl.DeviceIdType.MESH
VMEM_LIMIT = 67043328
SPARE = 64 * 1024
LANES = 128


def dot(a, b):
    return jnp.dot(a, b, preferred_element_type=F32)


def dot_nt(a, b):
    return lax.dot_general(a, b, (((1,), (1,)), ((), ())), preferred_element_type=F32)


def split(v):
    high = v.astype(BF16)
    return high, (v - high.astype(F32)).astype(BF16)


def softplus(v):
    return jnp.maximum(v, 0.0) + jnp.log1p(jnp.exp(-jnp.abs(v)))


def far_first(n):
    return sorted(range(n), key=lambda k: -min(k, n - k))


def loop(low, high, act):
    if high - low <= 32:
        for k in range(low, high):
            act(k)
        return

    def body(k, carry):
        act(k)
        return carry

    lax.fori_loop(low, high, body, 0)


def layer_kernel(
    n_ep,
    n_tp,
    tokens_hbm,
    routes_hbm,
    share_hbm,
    mgain_hbm,
    gate_hbm,
    input_hbm,
    step_hbm,
    write_hbm,
    read_hbm,
    bias_hbm,
    rate_hbm,
    jolt_hbm,
    taps_hbm,
    filter_hbm,
    state_hbm,
    skip_hbm,
    hgain_hbm,
    outw_hbm,
    cgain_hbm,
    egate_hbm,
    eup_hbm,
    edown_hbm,
    sgate_hbm,
    sup_hbm,
    sdown_hbm,
    out_ref,
    new_ref,
    new_filter_ref,
    tokens_ref,
    routes_ref,
    rweight_ref,
    mgain_ref,
    gate_ref,
    input_ref,
    step_ref,
    vecw_ref,
    bias_ref,
    rate_ref,
    jolt_ref,
    taps_ref,
    filter_ref,
    skip_ref,
    hgain_ref,
    outw_ref,
    cgain_ref,
    wgate_ref,
    wup_ref,
    wdown_ref,
    normed_buf,
    vec_out,
    vec_in,
    half_buf,
    column_buf,
    write_buf,
    part_buf,
    mix_buf,
    resid_buf,
    share_buf,
    acc_buf,
    hidden_buf,
    cross_out,
    cross_in,
    own_buf,
    term_buf,
    back_buf,
    load_sem,
    wide_sem,
    vec_send,
    vec_recv,
    mix_send,
    mix_recv,
    share_send,
    share_recv,
    resid_send,
    pass_send,
    resid_recv,
    cross_send,
    cross_recv,
    back_send,
    back_recv,
):
    ep = lax.axis_index("ep")
    tp = lax.axis_index("tp")
    core = lax.rem(tp, 2)
    z = tp // 2
    n_z = n_tp // 2
    n_same = n_ep * n_z
    partner = tp + 1 - 2 * core
    rows, model = tokens_ref.shape
    columns = out_ref.shape[1]
    heads = bias_ref.shape[1]
    width = gate_ref.shape[1]
    all_rows = n_ep * rows
    local = egate_hbm.shape[0]
    experts = local + 1
    units = wgate_ref.shape[-1]
    features = write_hbm.shape[0]
    group_lanes = GROUPS * STATE

    small = [
        (tokens_hbm, tokens_ref),
        (mgain_hbm, mgain_ref),
        (write_hbm, vecw_ref.at[:, :group_lanes]),
        (read_hbm, vecw_ref.at[:, group_lanes:]),
        (step_hbm, step_ref),
        (input_hbm, input_ref),
        (gate_hbm, gate_ref),
        (bias_hbm, bias_ref),
        (rate_hbm, rate_ref),
        (jolt_hbm, jolt_ref),
        (taps_hbm, taps_ref),
        (filter_hbm, filter_ref),
        (skip_hbm, skip_ref),
        (hgain_hbm, hgain_ref),
        (routes_hbm, routes_ref),
        (share_hbm, rweight_ref),
        (state_hbm, new_ref),
        (outw_hbm, outw_ref),
        (cgain_hbm, cgain_ref),
    ]
    loads = [
        pltpu.make_async_copy(src, dst, load_sem.at[i]) for i, (src, dst) in enumerate(small)
    ]
    wide = []
    for j in range(experts):
        for h in range(2):
            if j < local:
                wide.append((egate_hbm.at[j, :, h], wgate_ref.at[j, h]))
                wide.append((eup_hbm.at[j, :, h], wup_ref.at[j, h]))
            else:
                wide.append((sgate_hbm.at[:, h], wgate_ref.at[j, h]))
                wide.append((sup_hbm.at[:, h], wup_ref.at[j, h]))
    for j in range(experts):
        src = edown_hbm.at[j] if j < local else sdown_hbm
        wide.append((src, wdown_ref.at[pl.ds(j * units, units)]))
    wide = [pltpu.make_async_copy(src, dst, wide_sem.at[i]) for i, (src, dst) in enumerate(wide)]
    downs = wide[-experts:]
    ups = wide[:-experts]

    barrier = pltpu.get_barrier_semaphore()
    for k in range(1, n_tp):
        pl.semaphore_signal(
            barrier, inc=1, device_id=(ep, lax.rem(tp + k, n_tp)), device_id_type=MESH
        )
    for k in range(1, n_ep):
        pl.semaphore_signal(
            barrier, inc=1, device_id=(lax.rem(ep + k, n_ep), tp), device_id_type=MESH
        )
    for load in loads[:16]:
        load.start()

    def remote(src, dst, send, recv, device):
        return pltpu.make_async_remote_copy(
            src_ref=src,
            dst_ref=dst,
            send_sem=send,
            recv_sem=recv,
            device_id=device,
            device_id_type=MESH,
        )

    tp_order = [k for k in far_first(n_tp) if k]

    def tp_peer(k):
        return lax.rem(tp + k, n_tp)

    per_group = HEADS // GROUPS

    def vec_copy(k):
        peer = tp_peer(k)
        group = (peer * heads) // per_group
        return remote(
            vec_out.at[group], vec_in.at[tp], vec_send.at[k], vec_recv.at[tp], (ep, peer)
        )

    def vec_from(k):
        peer = tp_peer(k)
        return remote(
            vec_out.at[0], vec_in.at[peer], vec_send.at[k], vec_recv.at[peer], (ep, peer)
        )

    def share_copy(k):
        peer = lax.rem(ep + k, n_ep)
        return remote(
            share_buf.at[ep], share_buf.at[ep], share_send.at[k], share_recv.at[ep], (peer, tp)
        )

    def share_from(k):
        peer = lax.rem(ep + k, n_ep)
        return remote(
            share_buf.at[peer], share_buf.at[peer], share_send.at[k], share_recv.at[peer], (peer, tp)
        )

    def mix_copy(k):
        peer = tp_peer(k)
        return remote(
            part_buf.at[peer], mix_buf.at[tp], mix_send.at[k], mix_recv.at[tp], (ep, peer)
        )

    def mix_from(k):
        peer = tp_peer(k)
        return remote(
            part_buf.at[peer], mix_buf.at[peer], mix_send.at[k], mix_recv.at[peer], (ep, peer)
        )

    loads[0].wait()
    loads[1].wait()
    tokens = tokens_ref[...].astype(F32)
    scale = lax.rsqrt(jnp.mean(tokens * tokens, axis=-1, keepdims=True) + EPS)
    normed_buf[...] = (tokens * scale * mgain_ref[...]).astype(BF16)
    own = normed_buf[:, pl.ds(pl.multiple_of(tp * features, features), features)]
    loads[2].wait()
    loads[3].wait()
    vec_part = dot(own, vecw_ref[...]).astype(BF16)
    for g in range(GROUPS):
        at = slice(g * STATE, (g + 1) * STATE)
        vec_out[g, :, :STATE] = vec_part[:, at]
        vec_out[g, :, STATE:] = vec_part[:, group_lanes + g * STATE : group_lanes + (g + 1) * STATE]
    pl.semaphore_wait(barrier, n_tp - 1 + n_ep - 1)
    for k in tp_order:
        vec_copy(k).start()
    for load in loads[16:]:
        load.start()
    vec_in[tp] = vec_out[(tp * heads) // per_group]

    normed = normed_buf[...]
    loads[4].wait()
    step_raw = dot_nt(normed, step_ref[...])
    loads[5].wait()
    inputs = dot(normed, input_ref[...]).astype(BF16)
    loads[6].wait()
    gate_rows = dot(normed, gate_ref[...]).astype(BF16)
    for load in loads[7:16]:
        load.wait()
    taps = taps_ref[...].astype(F32)
    last = filter_ref.shape[0]
    total = inputs.astype(F32) * taps[last : last + 1]
    for i in range(last):
        total = total + filter_ref[i].astype(F32) * taps[i : i + 1]
        new_filter_ref[i] = filter_ref[i + 1] if i + 1 < last else inputs
    filtered = jax.nn.silu(total)
    jolt = jnp.transpose(
        jnp.concatenate([jolt_ref[...], jnp.zeros((heads, LANES - rows), F32)], axis=1)
    )[:rows]
    step = softplus(step_raw + bias_ref[...])
    decay = jnp.exp(jolt - jnp.exp(rate_ref[...]) * step)
    skip = jnp.broadcast_to(skip_ref[...], (rows, heads))
    stacked = jnp.concatenate([step, decay, skip], axis=0)
    head_lane = lax.broadcasted_iota(jnp.int32, (heads, width), 1) // HEAD_DIM
    spread = jnp.where(
        head_lane == lax.broadcasted_iota(jnp.int32, (heads, width), 0), 1.0, 0.0
    ).astype(BF16)
    high, low = split(stacked)
    expanded = dot(high, spread) + dot(low, spread)
    decay_row = expanded[rows : 2 * rows]
    x_row = expanded[:rows] * filtered
    direct = expanded[2 * rows :] * filtered
    gate_silu = jax.nn.silu(gate_rows.astype(F32))
    column_buf[...] = jnp.transpose(
        jnp.concatenate([x_row, decay_row, jnp.zeros((LANES - 2 * rows, width), F32)], axis=0)
    )

    ids = lax.broadcasted_iota(jnp.int32, (LANES, rows), 0)
    share = jnp.zeros((LANES, rows), F32)
    for k in range(routes_ref.shape[0]):
        share = share + jnp.where(
            routes_ref[k : k + 1, :] == ids, rweight_ref[k : k + 1, :], 0.0
        )
    share_buf[ep] = jnp.transpose(
        jnp.concatenate([share, jnp.zeros((LANES, LANES - rows), F32)], axis=1)
    )[:rows]
    for k in range(1, n_ep):
        share_copy(k).start()

    loads[16].wait()
    for s in range(rows):
        half_buf[:, s * STATE : (s + 1) * STATE] = new_ref[s].astype(BF16)

    for k in reversed(tp_order):
        vec_from(k).wait_recv()
    for load in ups:
        load.start()
    for load in downs:
        load.start()
    vecs = jax.nn.silu(jnp.sum(vec_in[...].astype(F32), axis=0))
    write = vecs[:, :STATE]
    read = vecs[:, STATE:]
    write_buf[...] = write
    row_ids = lax.broadcasted_iota(jnp.int32, (rows, STATE), 0)
    spread_read = jnp.concatenate(
        [jnp.where(row_ids == s, read, 0.0).astype(BF16) for s in range(rows)], axis=1
    )
    state_read = dot_nt(spread_read, half_buf[...])
    overlap = jnp.sum(write * read, axis=1, keepdims=True)
    value = (decay_row * state_read + x_row * overlap + direct) * gate_silu
    same = (
        lax.broadcasted_iota(jnp.int32, (LANES, LANES), 0) // HEAD_DIM
        == lax.broadcasted_iota(jnp.int32, (LANES, LANES), 1) // HEAD_DIM
    )
    block = jnp.where(same, 1.0 / HEAD_DIM, 0.0).astype(BF16)
    pieces = width // LANES
    square = (value * value).astype(BF16)
    means = dot(
        jnp.concatenate([square[:, j * LANES : (j + 1) * LANES] for j in range(pieces)], axis=0),
        block,
    )
    mean_square = jnp.concatenate(
        [means[j * rows : (j + 1) * rows] for j in range(pieces)], axis=1
    )
    gated = (value * lax.rsqrt(mean_square + EPS) * hgain_ref[...]).astype(BF16)
    loads[17].wait()

    def part_of(t):
        return dot(
            gated, outw_ref[:, pl.ds(pl.multiple_of(t * columns, columns), columns)]
        ).astype(BF16)

    for k in tp_order:
        peer = tp_peer(k)
        part_buf[peer] = part_of(peer)
        mix_copy(k).start()
    mix_buf[tp] = part_of(tp)

    for s in range(rows):
        new_ref[s] = (
            column_buf[:, rows + s : rows + s + 1] * new_ref[s]
            + column_buf[:, s : s + 1] * write_buf[s : s + 1, :]
        )

    own_tokens = tokens_ref[:, pl.ds(pl.multiple_of(tp * columns, columns), columns)]
    for k in reversed(tp_order):
        mix_from(k).wait_recv()
    mixed = jnp.sum(mix_buf[...].astype(F32), axis=0).astype(BF16)
    resid_buf[core, z, ep] = (own_tokens.astype(F32) + mixed.astype(F32)).astype(BF16)

    def place(m):
        return lax.rem(ep + m // n_z, n_ep), lax.rem(z + m % n_z, n_z)

    def resid_copy(m):
        e, zz = place(m)
        here = resid_buf.at[core, z, ep]
        return remote(
            here,
            here,
            resid_send.at[m],
            resid_recv.at[core, z * n_ep + ep],
            (e, zz * 2 + core),
        )

    def resid_from(m):
        e, zz = place(m)
        there = resid_buf.at[core, zz, e]
        return remote(
            there, there, resid_send.at[m], resid_recv.at[core, zz * n_ep + e], (e, zz * 2 + core)
        )

    def pass_copy(m):
        e, zz = place(m)
        there = resid_buf.at[core, zz, e]
        return remote(
            there, there, pass_send.at[m], resid_recv.at[core, zz * n_ep + e], (ep, partner)
        )

    def pass_from(m):
        e, zz = place(m)
        there = resid_buf.at[1 - core, zz, e]
        return remote(
            there, there, pass_send.at[m], resid_recv.at[1 - core, zz * n_ep + e], (ep, partner)
        )

    loop(1, n_same, lambda k: resid_copy(n_same - k).start())
    pass_copy(0).start()
    loads[18].wait()
    for k in range(1, n_ep):
        share_from(k).wait_recv()
    shares = share_buf[...].reshape(all_rows, LANES)
    all_lanes = lax.broadcasted_iota(jnp.int32, shares.shape, 1)
    own_rows = lax.broadcasted_iota(jnp.int32, (all_rows, 1), 0) // rows == ep
    scales = [
        jnp.sum(jnp.where(all_lanes == ep * local + j, shares, 0.0), axis=1, keepdims=True)
        for j in range(local)
    ] + [jnp.where(own_rows, 1.0, 0.0)]
    for load in ups:
        load.wait()

    def relay(m):
        resid_from(m).wait_recv()
        pass_copy(m).start()

    loop(1, n_same, relay)

    def half(h):
        square = jnp.zeros((all_rows, columns), F32)
        scaled = []
        for zz in range(n_z):
            part = resid_buf[h, zz].reshape(all_rows, columns).astype(F32)
            square = square + part * part
            at = pl.multiple_of((zz * 2 + h) * columns, columns)
            scaled.append((part * cgain_ref[:, pl.ds(at, columns)]).astype(BF16))
        scaled = jnp.concatenate(scaled, axis=1)
        sums = []
        for j in range(experts):
            for weights in (wgate_ref, wup_ref):
                sums.append(dot(scaled, weights[j, h].reshape(n_z * columns, units)))
        return square, sums

    square, sums = half(core)
    for i, value in enumerate(sums):
        acc_buf[i] = value
    loop(0, n_same, lambda m: pass_from(m).wait_recv())
    square_two, sums = half(1 - core)
    mean_square = jnp.sum(square + square_two, axis=-1, keepdims=True) * (1.0 / model)
    scale = lax.rsqrt(mean_square + EPS)
    for j in range(experts):
        gate = (acc_buf[2 * j] + sums[2 * j]) * scale
        up = (acc_buf[2 * j + 1] + sums[2 * j + 1]) * scale
        hidden_buf[:, j * units : (j + 1) * units] = (
            jax.nn.silu(gate) * up * scales[j]
        ).astype(BF16)
    for load in downs:
        load.wait()
    hidden = hidden_buf[...]

    def down_of(t):
        return dot(hidden, wdown_ref[:, pl.ds(pl.multiple_of(t * columns, columns), columns)])

    def cross_copy(zz):
        return remote(
            cross_out.at[zz], cross_in.at[zz], cross_send.at[zz], cross_recv.at[zz], (ep, partner)
        )

    z_order = [lax.rem(z + k, n_z) for k in far_first(n_z)]
    for zz in z_order:
        cross_out[zz] = down_of(zz * 2 + 1 - core).astype(BF16)
        cross_copy(zz).start()
    for zz in z_order:
        own_buf[zz] = down_of(zz * 2 + core)

    def back_copy(zz, e, m):
        return remote(
            term_buf.at[zz, e],
            back_buf.at[ep * n_z + z],
            back_send.at[m],
            back_recv.at[ep * n_z + z],
            (e, zz * 2 + core),
        )

    def back_from(m):
        e, zz = place(m)
        return remote(
            term_buf.at[zz, e],
            back_buf.at[e * n_z + zz],
            back_send.at[m],
            back_recv.at[e * n_z + zz],
            (e, zz * 2 + core),
        )

    for i, k in enumerate(far_first(n_z)):
        zz = z_order[i]
        cross_copy(zz).wait_recv()
        term_buf[zz] = (own_buf[zz] + cross_in[zz].astype(F32)).astype(BF16).reshape(
            n_ep, rows, columns
        )
        for step_ep in range(n_ep - 1, -1, -1):
            if k or step_ep:
                back_copy(zz, lax.rem(ep + step_ep, n_ep), step_ep * n_z + k).start()
    back_buf[ep * n_z + z] = term_buf[z, ep]
    loop(1, n_same, lambda m: back_from(m).wait_recv())
    out_ref[...] = (
        resid_buf[core, z, ep].astype(F32) + jnp.sum(back_buf[...].astype(F32), axis=0)
    ).astype(BF16)

    for k in tp_order:
        vec_copy(k).wait_send()
        mix_copy(k).wait_send()
    for k in range(1, n_ep):
        share_copy(k).wait_send()
    loop(1, n_same, lambda m: resid_copy(m).wait_send())
    loop(0, n_same, lambda m: pass_copy(m).wait_send())
    for zz in range(n_z):
        cross_copy(zz).wait_send()
    loop(1, n_same, lambda m: back_from(m).wait_send())


def finish_kernel(out_in, new_in, filter_in, out_ref, new_ref, filter_ref, sem):
    pairs = ((new_in, new_ref), (out_in, out_ref), (filter_in, filter_ref))
    copies = [pltpu.make_async_copy(src, dst, sem.at[i]) for i, (src, dst) in enumerate(pairs)]
    for copy in copies:
        copy.start()
    for copy in copies:
        copy.wait()


def on_device(
    tokens,
    routes,
    route_weight,
    mixer_gain,
    gate_weight,
    input_weight,
    step_weight,
    write_weight,
    read_weight,
    step_bias,
    decay_log,
    decay_jolt,
    filter_taps,
    filter_state,
    scan_state,
    skip_gain,
    head_gain,
    output_weight,
    channel_gain,
    expert_gate,
    expert_up,
    expert_down,
    shared_gate,
    shared_up,
    shared_down,
):
    rows, model = tokens.shape
    n_tp = lax.axis_size("tp")
    n_ep = lax.axis_size("ep")
    n_z = n_tp // 2
    n_same = n_ep * n_z
    columns = model // n_tp
    heads_here = step_bias.shape[0]
    width = gate_weight.shape[1]
    local, _, units = expert_gate.shape
    experts = local + 1
    taps = filter_state.shape[1]
    hbm = pl.BlockSpec(memory_space=pl.ANY)
    vmem = pl.BlockSpec(memory_space=pltpu.VMEM)
    dma = pltpu.SemaphoreType.DMA
    shape = jax.ShapeDtypeStruct
    outs = (
        shape((rows, columns), BF16),
        shape((rows, width, STATE), F32),
        shape((taps, rows, width), BF16),
    )
    operands = (
        tokens,
        routes.T,
        route_weight.T,
        mixer_gain.reshape(1, model),
        gate_weight,
        input_weight,
        step_weight.T,
        write_weight,
        read_weight,
        step_bias.reshape(1, heads_here),
        decay_log.reshape(1, heads_here),
        decay_jolt.T,
        filter_taps,
        jnp.transpose(filter_state, (1, 0, 2)),
        scan_state.reshape(rows, width, STATE),
        skip_gain.reshape(1, heads_here),
        head_gain.reshape(1, width),
        output_weight,
        channel_gain.reshape(1, model),
        expert_gate.reshape(local, n_z, 2, columns, units),
        expert_up.reshape(local, n_z, 2, columns, units),
        expert_down,
        shared_gate.reshape(n_z, 2, columns, units),
        shared_up.reshape(n_z, 2, columns, units),
        shared_down,
    )
    vm = pltpu.VMEM
    held = [
        vm(operands[0].shape, BF16),
        vm(operands[1].shape, jnp.int32),
        vm(operands[2].shape, F32),
        vm(operands[3].shape, F32),
        vm(gate_weight.shape, BF16),
        vm(input_weight.shape, BF16),
        vm(operands[6].shape, BF16),
        vm((write_weight.shape[0], 2 * GROUPS * STATE), BF16),
        vm((1, heads_here), F32),
        vm((1, heads_here), F32),
        vm(operands[11].shape, F32),
        vm(filter_taps.shape, BF16),
        vm(operands[13].shape, BF16),
        vm((1, heads_here), F32),
        vm((1, width), F32),
        vm(output_weight.shape, BF16),
        vm((1, model), F32),
        vm((experts, 2, n_z, columns, units), BF16),
        vm((experts, 2, n_z, columns, units), BF16),
        vm((experts * units, model), BF16),
    ]
    layer_out, new_state, new_filter = pl.pallas_call(
        functools.partial(layer_kernel, n_ep, n_tp),
        out_shape=tuple(vm(out.shape, out.dtype) for out in outs),
        in_specs=[hbm] * len(operands),
        out_specs=(vmem,) * 3,
        scratch_shapes=held
        + [
            vm((rows, model), BF16),
            vm((GROUPS, rows, 2 * STATE), BF16),
            vm((n_tp, rows, 2 * STATE), BF16),
            vm((width, rows * STATE), BF16),
            vm((width, LANES), F32),
            vm((rows, STATE), F32),
            vm((n_tp, rows, columns), BF16),
            vm((n_tp, rows, columns), BF16),
            vm((2, n_z, n_ep, rows, columns), BF16),
            vm((n_ep, rows, LANES), F32),
            vm((2 * experts, n_ep * rows, units), F32),
            vm((n_ep * rows, experts * units), BF16),
            vm((n_z, n_ep * rows, columns), BF16),
            vm((n_z, n_ep * rows, columns), BF16),
            vm((n_z, n_ep * rows, columns), F32),
            vm((n_z, n_ep, rows, columns), BF16),
            vm((n_same, rows, columns), BF16),
            dma((19,)),
            dma((5 * experts,)),
            dma((n_tp,)),
            dma((n_tp,)),
            dma((n_tp,)),
            dma((n_tp,)),
            dma((n_ep,)),
            dma((n_ep,)),
            dma((n_same,)),
            dma((n_same,)),
            dma((2, n_same)),
            dma((n_z,)),
            dma((n_z,)),
            dma((n_same,)),
            dma((n_same,)),
        ],
        compiler_params=pltpu.CompilerParams(
            collective_id=0,
            has_side_effects=True,
            vmem_limit_bytes=VMEM_LIMIT - 4 * rows * width * STATE - SPARE,
        ),
        name="layer",
    )(*operands)
    layer_out, new_state, new_filter = pl.pallas_call(
        finish_kernel,
        out_shape=outs,
        in_specs=[vmem] * 3,
        out_specs=(hbm,) * 3,
        scratch_shapes=[dma((3,))],
        compiler_params=pltpu.CompilerParams(vmem_limit_bytes=1024 * 1024),
        name="finish",
    )(layer_out, new_state, new_filter)
    return (
        layer_out,
        new_state.reshape(scan_state.shape),
        jnp.transpose(new_filter, (1, 0, 2)),
    )


def solution(mesh):
    in_specs = (
        P("ep", None),
        P("ep", None),
        P("ep", None),
        P(),
        P(None, "tp"),
        P(None, "tp"),
        P(None, "tp"),
        P("tp", None),
        P("tp", None),
        P("tp"),
        P("tp"),
        P("ep", "tp"),
        P(None, "tp"),
        P("ep", None, "tp"),
        P("ep", "tp", None, None),
        P("tp"),
        P("tp"),
        P("tp", None),
        P(),
        P("ep", None, "tp"),
        P("ep", None, "tp"),
        P("ep", "tp", None),
        P(None, "tp"),
        P(None, "tp"),
        P("tp", None),
    )
    out_specs = (P("ep", "tp"), P("ep", "tp", None, None), P("ep", None, "tp"))
    return jax.shard_map(
        on_device, mesh=mesh, in_specs=in_specs, out_specs=out_specs, check_vma=False
    )
```

```python
import functools

import jax
import jax.numpy as jnp
from jax import lax
from jax.experimental import pallas as pl
from jax.experimental.pallas import tpu as pltpu
from jax.sharding import PartitionSpec as P

HEADS = 64
HEAD_DIM = 64
GROUPS = 4
STATE = 128

EPS = 1e-06
F32 = jnp.float32
BF16 = jnp.bfloat16
MESH = pl.DeviceIdType.MESH
VMEM_LIMIT = 67043328
SPARE = 64 * 1024
LANES = 128


def dot(a, b):
    return jnp.dot(a, b, preferred_element_type=F32)


def dot_nt(a, b):
    return lax.dot_general(a, b, (((1,), (1,)), ((), ())), preferred_element_type=F32)


def split(v):
    high = v.astype(BF16)
    return high, (v - high.astype(F32)).astype(BF16)


def softplus(v):
    return jnp.maximum(v, 0.0) + jnp.log1p(jnp.exp(-jnp.abs(v)))


def far_first(n):
    return sorted(range(n), key=lambda k: -min(k, n - k))


def layer_kernel(
    n_ep,
    n_tp,
    tokens_hbm,
    routes_hbm,
    share_hbm,
    mgain_hbm,
    gate_hbm,
    input_hbm,
    step_hbm,
    write_hbm,
    read_hbm,
    bias_hbm,
    rate_hbm,
    jolt_hbm,
    taps_hbm,
    filter_hbm,
    state_hbm,
    skip_hbm,
    hgain_hbm,
    outw_hbm,
    cgain_hbm,
    egate_hbm,
    eup_hbm,
    edown_hbm,
    sgate_hbm,
    sup_hbm,
    sdown_hbm,
    out_ref,
    new_ref,
    new_filter_ref,
    tokens_ref,
    routes_ref,
    rweight_ref,
    mgain_ref,
    gate_ref,
    input_ref,
    step_ref,
    vecw_ref,
    bias_ref,
    rate_ref,
    jolt_ref,
    taps_ref,
    filter_ref,
    skip_ref,
    hgain_ref,
    outw_ref,
    cgain_ref,
    wide_ref,
    down_ref,
    normed_buf,
    vec_out,
    vec_in,
    half_buf,
    column_buf,
    write_buf,
    part_buf,
    mix_in,
    resid_buf,
    share_buf,
    acc_buf,
    hidden_buf,
    cross_out,
    cross_in,
    own_buf,
    term_buf,
    back_in,
    load_sem,
    send_sem,
    recv_sem,
    direct_recv,
    pass_recv,
    cross_recv,
):
    ep = lax.axis_index("ep")
    tp = lax.axis_index("tp")
    core = lax.rem(tp, 2)
    z = tp // 2
    n_z = n_tp // 2
    n_same = n_ep * n_z
    partner = tp + 1 - 2 * core
    rows, model = tokens_ref.shape
    columns = out_ref.shape[1]
    heads = bias_ref.shape[1]
    width = gate_ref.shape[1]
    all_rows = n_ep * rows
    local = egate_hbm.shape[0]
    experts = local + 1
    units = edown_hbm.shape[1]
    features = write_hbm.shape[0]
    group_lanes = GROUPS * STATE
    per_group = HEADS // GROUPS
    tp_order = [k for k in far_first(n_tp) if k] + [0]
    z_far = far_first(n_z)
    z_near = z_far[::-1]

    def tp_peer(k):
        return lax.rem(tp + k, n_tp)

    def ep_peer(k):
        return lax.rem(ep + k, n_ep)

    def z_peer(k):
        return lax.rem(z + k, n_z)

    def block(t, size):
        return pl.ds(pl.multiple_of(t * size, size), size)

    def loaded(i, dst):
        return pltpu.make_async_copy(dst, dst, load_sem.at[i])

    singles = [
        (tokens_hbm, tokens_ref),
        (mgain_hbm, mgain_ref),
        (write_hbm, vecw_ref.at[:, :group_lanes]),
        (read_hbm, vecw_ref.at[:, group_lanes:]),
        (step_hbm, step_ref),
        (input_hbm, input_ref),
        (gate_hbm, gate_ref),
        (bias_hbm, bias_ref),
        (rate_hbm, rate_ref),
        (jolt_hbm, jolt_ref),
        (taps_hbm, taps_ref),
        (filter_hbm, filter_ref),
        (skip_hbm, skip_ref),
        (hgain_hbm, hgain_ref),
        (routes_hbm, routes_ref),
        (share_hbm, rweight_ref),
        (state_hbm, new_ref),
        (cgain_hbm, cgain_ref),
    ]
    loads = [
        pltpu.make_async_copy(src, dst, load_sem.at[i if i != 3 else 2])
        for i, (src, dst) in enumerate(singles)
    ]
    outw_sem, wide_sem, down_sem = 3, 18, 19
    outw_loads = [
        pltpu.make_async_copy(
            outw_hbm.at[:, block(tp_peer(k), columns)],
            outw_ref.at[:, i * columns : (i + 1) * columns],
            load_sem.at[outw_sem],
        )
        for i, k in enumerate(tp_order)
    ]
    wide_loads = []
    for side in range(2):
        for k in z_near:
            t = z_peer(k) * 2 + (1 - core if side == 0 else core)
            for j in range(experts):
                for g, (routed, shared) in enumerate(
                    ((egate_hbm, sgate_hbm), (eup_hbm, sup_hbm))
                ):
                    source = routed.at[j] if j < local else shared
                    lane = (2 * j + g) * units
                    wide_loads.append(
                        pltpu.make_async_copy(
                            source.at[block(t, columns)],
                            wide_ref.at[side, k, :, lane : lane + units],
                            load_sem.at[wide_sem],
                        )
                    )
    down_loads = []
    for side in range(2):
        for i, k in enumerate(z_far):
            t = z_peer(k) * 2 + (core if side == 0 else 1 - core)
            for j in range(experts):
                source = edown_hbm.at[j] if j < local else sdown_hbm
                down_loads.append(
                    pltpu.make_async_copy(
                        source.at[:, block(t, columns)],
                        down_ref.at[
                            side,
                            j * units : (j + 1) * units,
                            i * columns : (i + 1) * columns,
                        ],
                        load_sem.at[down_sem],
                    )
                )

    barrier = pltpu.get_barrier_semaphore()
    for k in range(1, n_tp):
        pl.semaphore_signal(barrier, inc=1, device_id=(ep, tp_peer(k)), device_id_type=MESH)
    for k in range(1, n_ep):
        pl.semaphore_signal(barrier, inc=1, device_id=(ep_peer(k), tp), device_id_type=MESH)
    for load in loads[:16]:
        load.start()

    def remote(src, dst, send, recv, device):
        return pltpu.make_async_remote_copy(
            src_ref=src,
            dst_ref=dst,
            send_sem=send_sem.at[send],
            recv_sem=recv,
            device_id=device,
            device_id_type=MESH,
        )

    VEC, SHARE, MIX, RESID, PASS, CROSS, BACK = range(7)
    vec_recv, share_recv, mix_recv, back_recv = (recv_sem.at[i] for i in range(4))

    def vec_copy(k):
        peer = tp_peer(k)
        group = (peer * heads) // per_group
        return remote(vec_out.at[group], vec_in.at[k - 1], VEC, vec_recv, (ep, peer))

    def share_copy(k):
        target = (lax.rem(ep + n_ep - k, n_ep), tp)
        return remote(share_buf.at[0], share_buf.at[k], SHARE, share_recv, target)

    def mix_copy(i, k):
        return remote(part_buf.at[i], mix_in.at[k - 1], MIX, mix_recv, (ep, tp_peer(k)))

    def resid_copy(e, k):
        here = resid_buf.at[1, 0, 0]
        target = (lax.rem(ep + n_ep - e, n_ep), lax.rem(z + n_z - k, n_z) * 2 + 1 - core)
        return remote(here, resid_buf.at[0, k, e], RESID, direct_recv.at[k], target)

    def pass_copy(k):
        at = pl.ds(0 if k else 1, n_ep if k else n_ep - 1)
        return remote(
            resid_buf.at[0, k, at], resid_buf.at[1, k, at], PASS, pass_recv.at[k], (ep, partner)
        )

    half_z = n_z // 2

    def cross_copy(i):
        at = pl.ds(i * half_z, half_z)
        return remote(cross_out.at[at], cross_in.at[at], CROSS, cross_recv.at[i], (ep, partner))

    def back_copy(i, e, k):
        target = (ep_peer(e), z_peer(k) * 2 + 1 - core)
        return remote(term_buf.at[i, e], back_in.at[e * n_z + k], BACK, back_recv, target)

    def whole(buf, send, recv):
        return remote(buf, buf, send, recv, (ep, partner))

    loads[0].wait()
    loads[1].wait()
    tokens = tokens_ref[...].astype(F32)
    scale = lax.rsqrt(jnp.mean(tokens * tokens, axis=-1, keepdims=True) + EPS)
    normed_buf[...] = (tokens * scale * mgain_ref[...]).astype(BF16)
    own = normed_buf[:, block(tp, features)]
    loaded(2, vecw_ref).wait()
    vec_part = dot(own, vecw_ref[...]).astype(BF16)
    for g in range(GROUPS):
        at = slice(g * STATE, (g + 1) * STATE)
        vec_out[g, :, :STATE] = vec_part[:, at]
        vec_out[g, :, STATE:] = vec_part[:, group_lanes + g * STATE : group_lanes + (g + 1) * STATE]
    pl.semaphore_wait(barrier, n_tp - 1 + n_ep - 1)
    for k in tp_order[:-1]:
        vec_copy(k).start()
    loads[16].start()
    for load in outw_loads:
        load.start()
    loads[17].start()

    normed = normed_buf[...]
    loads[4].wait()
    step_raw = dot_nt(normed, step_ref[...])
    loads[5].wait()
    inputs = dot(normed, input_ref[...]).astype(BF16)
    loads[6].wait()
    gate_rows = dot(normed, gate_ref[...]).astype(BF16)
    for load in loads[7:16]:
        load.wait()
    taps = taps_ref[...].astype(F32)
    last = filter_ref.shape[0]
    total = inputs.astype(F32) * taps[last : last + 1]
    for i in range(last):
        total = total + filter_ref[i].astype(F32) * taps[i : i + 1]
        new_filter_ref[i] = filter_ref[i + 1] if i + 1 < last else inputs
    filtered = jax.nn.silu(total)
    jolt = jnp.transpose(
        jnp.concatenate([jolt_ref[...], jnp.zeros((heads, LANES - rows), F32)], axis=1)
    )[:rows]
    step = softplus(step_raw + bias_ref[...])
    decay = jnp.exp(jolt - jnp.exp(rate_ref[...]) * step)
    skip = jnp.broadcast_to(skip_ref[...], (rows, heads))
    stacked = jnp.concatenate([step, decay, skip], axis=0)
    head_lane = lax.broadcasted_iota(jnp.int32, (heads, width), 1) // HEAD_DIM
    spread = jnp.where(
        head_lane == lax.broadcasted_iota(jnp.int32, (heads, width), 0), 1.0, 0.0
    ).astype(BF16)
    high, low = split(stacked)
    expanded = dot(high, spread) + dot(low, spread)
    decay_row = expanded[rows : 2 * rows]
    x_row = expanded[:rows] * filtered
    direct = expanded[2 * rows :] * filtered
    gate_silu = jax.nn.silu(gate_rows.astype(F32))
    column_buf[...] = jnp.transpose(
        jnp.concatenate([x_row, decay_row, jnp.zeros((LANES - 2 * rows, width), F32)], axis=0)
    )

    ids = lax.broadcasted_iota(jnp.int32, (LANES, rows), 0)
    share = jnp.zeros((LANES, rows), F32)
    for k in range(routes_ref.shape[0]):
        share = share + jnp.where(
            routes_ref[k : k + 1, :] == ids, rweight_ref[k : k + 1, :], 0.0
        )
    share_buf[0] = jnp.transpose(
        jnp.concatenate([share, jnp.zeros((LANES, LANES - rows), F32)], axis=1)
    )[:rows]
    for k in range(1, n_ep):
        share_copy(k).start()

    loads[16].wait()
    for s in range(rows):
        half_buf[:, s * STATE : (s + 1) * STATE] = new_ref[s].astype(BF16)

    for load in wide_loads:
        load.start()
    for load in down_loads:
        load.start()
    whole(vec_in, VEC, vec_recv).wait_recv()
    vecs = jax.nn.silu(
        vec_out[(tp * heads) // per_group].astype(F32)
        + jnp.sum(vec_in[...].astype(F32), axis=0)
    )
    write = vecs[:, :STATE]
    read = vecs[:, STATE:]
    write_buf[...] = write
    row_ids = lax.broadcasted_iota(jnp.int32, (rows, STATE), 0)
    spread_read = jnp.concatenate(
        [jnp.where(row_ids == s, read, 0.0).astype(BF16) for s in range(rows)], axis=1
    )
    state_read = dot_nt(spread_read, half_buf[...])
    overlap = jnp.sum(write * read, axis=1, keepdims=True)
    value = (decay_row * state_read + x_row * overlap + direct) * gate_silu
    same = (
        lax.broadcasted_iota(jnp.int32, (LANES, LANES), 0) // HEAD_DIM
        == lax.broadcasted_iota(jnp.int32, (LANES, LANES), 1) // HEAD_DIM
    )
    averaging = jnp.where(same, 1.0 / HEAD_DIM, 0.0).astype(BF16)
    pieces = width // LANES
    square = (value * value).astype(BF16)
    means = dot(
        jnp.concatenate([square[:, j * LANES : (j + 1) * LANES] for j in range(pieces)], axis=0),
        averaging,
    )
    mean_square = jnp.concatenate(
        [means[j * rows : (j + 1) * rows] for j in range(pieces)], axis=1
    )
    gated = (value * lax.rsqrt(mean_square + EPS) * hgain_ref[...]).astype(BF16)
    loaded(outw_sem, outw_ref).wait()
    half_tp = n_tp // 2
    for h in range(2):
        at = slice(h * half_tp * columns, (h + 1) * half_tp * columns)
        part = dot(gated, outw_ref[:, at]).astype(BF16)
        for i in range(half_tp):
            part_buf[h * half_tp + i] = part[:, i * columns : (i + 1) * columns]
        for i in range(half_tp):
            k = tp_order[h * half_tp + i]
            if k:
                mix_copy(h * half_tp + i, k).start()

    for s in range(rows):
        new_ref[s] = (
            column_buf[:, rows + s : rows + s + 1] * new_ref[s]
            + column_buf[:, s : s + 1] * write_buf[s : s + 1, :]
        )

    own_mix = tokens_ref[:, block(tp, columns)].astype(F32)
    whole(mix_in, MIX, mix_recv).wait_recv()
    mixed = (
        part_buf[n_tp - 1].astype(F32) + jnp.sum(mix_in[...].astype(F32), axis=0)
    ).astype(BF16)
    resid_buf[1, 0, 0] = (own_mix + mixed.astype(F32)).astype(BF16)
    for k in z_near:
        for e in range(n_ep - 1, -1, -1):
            resid_copy(e, k).start()

    loads[17].wait()
    whole(share_buf.at[pl.ds(1, n_ep - 1)], SHARE, share_recv).wait_recv()
    shares = share_buf[...].reshape(all_rows, LANES)
    all_lanes = lax.broadcasted_iota(jnp.int32, shares.shape, 1)
    own_rows = lax.broadcasted_iota(jnp.int32, (all_rows, 1), 0) < rows
    scales = [
        jnp.sum(jnp.where(all_lanes == ep * local + j, shares, 0.0), axis=1, keepdims=True)
        for j in range(local)
    ] + [jnp.where(own_rows, 1.0, 0.0)]
    loaded(wide_sem, wide_ref).wait()
    loaded(down_sem, down_ref).wait()

    squares = []

    def piece(side, k):
        part = resid_buf[side, k].reshape(all_rows, columns).astype(F32)
        squares.append(part * part)
        t = z_peer(k) * 2 + (1 - core if side == 0 else core)
        scaled = (part * cgain_ref[:, block(t, columns)]).astype(BF16)
        product = dot(scaled, wide_ref[side, k])
        if len(squares) == 1:
            acc_buf[...] = product
        else:
            acc_buf[...] += product

    def relay(k):
        whole(resid_buf.at[0, k], RESID, direct_recv.at[k]).wait_recv()
        pass_copy(k).start()
        piece(0, k)

    def passed(k):
        pass_copy(k).wait_recv()
        piece(1, k)

    for k in z_near[:-1]:
        relay(k)
    passed(z_near[0])
    relay(z_near[-1])
    for k in z_near[1:]:
        passed(k)
    square = squares[0]
    for other in squares[1:]:
        square = square + other
    scale = lax.rsqrt(jnp.sum(square, axis=-1, keepdims=True) * (1.0 / model) + EPS)
    for j in range(experts):
        gate = acc_buf[:, 2 * j * units : (2 * j + 1) * units] * scale
        up = acc_buf[:, (2 * j + 1) * units : (2 * j + 2) * units] * scale
        hidden_buf[:, j * units : (j + 1) * units] = (
            jax.nn.silu(gate) * up * scales[j]
        ).astype(BF16)
    hidden = hidden_buf[...]
    span = half_z * columns
    for h in range(2):
        result = dot(hidden, down_ref[0, :, h * span : (h + 1) * span]).astype(BF16)
        for i in range(half_z):
            cross_out[h * half_z + i] = result[:, i * columns : (i + 1) * columns]
        cross_copy(h).start()
    result = dot(hidden, down_ref[1])
    for i in range(n_z):
        own_buf[i] = result[:, i * columns : (i + 1) * columns]
    for h in range(2):
        cross_copy(h).wait_recv()
        for i in range(h * half_z, (h + 1) * half_z):
            k = z_far[i]
            term_buf[i] = (
                (own_buf[i] + cross_in[i].astype(F32)).astype(BF16).reshape(n_ep, rows, columns)
            )
            for e in range(n_ep - 1, -1, -1):
                back_copy(i, e, k).start()
    whole(back_in, BACK, back_recv).wait_recv()
    out_ref[...] = (
        resid_buf[1, 0, 0].astype(F32) + jnp.sum(back_in[...].astype(F32), axis=0)
    ).astype(BF16)

    whole(vec_in, VEC, vec_recv).wait_send()
    whole(share_buf.at[pl.ds(1, n_ep - 1)], SHARE, share_recv).wait_send()
    whole(mix_in, MIX, mix_recv).wait_send()
    whole(back_in, RESID, back_recv).wait_send()
    for k in range(n_z):
        pass_copy(k).wait_send()
    whole(cross_out, CROSS, back_recv).wait_send()
    whole(back_in, BACK, back_recv).wait_send()


def finish_kernel(out_in, new_in, filter_in, out_ref, new_ref, filter_ref, sem):
    pairs = ((new_in, new_ref), (out_in, out_ref), (filter_in, filter_ref))
    copies = [pltpu.make_async_copy(src, dst, sem.at[i]) for i, (src, dst) in enumerate(pairs)]
    for copy in copies:
        copy.start()
    for copy in copies:
        copy.wait()


def on_device(
    tokens,
    routes,
    route_weight,
    mixer_gain,
    gate_weight,
    input_weight,
    step_weight,
    write_weight,
    read_weight,
    step_bias,
    decay_log,
    decay_jolt,
    filter_taps,
    filter_state,
    scan_state,
    skip_gain,
    head_gain,
    output_weight,
    channel_gain,
    expert_gate,
    expert_up,
    expert_down,
    shared_gate,
    shared_up,
    shared_down,
):
    rows, model = tokens.shape
    n_tp = lax.axis_size("tp")
    n_ep = lax.axis_size("ep")
    n_z = n_tp // 2
    n_same = n_ep * n_z
    columns = model // n_tp
    heads_here = step_bias.shape[0]
    width = gate_weight.shape[1]
    local, _, units = expert_gate.shape
    experts = local + 1
    taps = filter_state.shape[1]
    hbm = pl.BlockSpec(memory_space=pl.ANY)
    vmem = pl.BlockSpec(memory_space=pltpu.VMEM)
    dma = pltpu.SemaphoreType.DMA
    shape = jax.ShapeDtypeStruct
    outs = (
        shape((rows, columns), BF16),
        shape((rows, width, STATE), F32),
        shape((taps, rows, width), BF16),
    )
    operands = (
        tokens,
        routes.T,
        route_weight.T,
        mixer_gain.reshape(1, model),
        gate_weight,
        input_weight,
        step_weight.T,
        write_weight,
        read_weight,
        step_bias.reshape(1, heads_here),
        decay_log.reshape(1, heads_here),
        decay_jolt.T,
        filter_taps,
        jnp.transpose(filter_state, (1, 0, 2)),
        scan_state.reshape(rows, width, STATE),
        skip_gain.reshape(1, heads_here),
        head_gain.reshape(1, width),
        output_weight,
        channel_gain.reshape(1, model),
        expert_gate,
        expert_up,
        expert_down,
        shared_gate,
        shared_up,
        shared_down,
    )
    vm = pltpu.VMEM
    held = [
        vm(operands[0].shape, BF16),
        vm(operands[1].shape, jnp.int32),
        vm(operands[2].shape, F32),
        vm(operands[3].shape, F32),
        vm(gate_weight.shape, BF16),
        vm(input_weight.shape, BF16),
        vm(operands[6].shape, BF16),
        vm((write_weight.shape[0], 2 * GROUPS * STATE), BF16),
        vm((1, heads_here), F32),
        vm((1, heads_here), F32),
        vm(operands[11].shape, F32),
        vm(filter_taps.shape, BF16),
        vm(operands[13].shape, BF16),
        vm((1, heads_here), F32),
        vm((1, width), F32),
        vm(output_weight.shape, BF16),
        vm((1, model), F32),
        vm((2, n_z, columns, 2 * experts * units), BF16),
        vm((2, experts * units, n_z * columns), BF16),
    ]
    layer_out, new_state, new_filter = pl.pallas_call(
        functools.partial(layer_kernel, n_ep, n_tp),
        out_shape=tuple(vm(out.shape, out.dtype) for out in outs),
        in_specs=[hbm] * len(operands),
        out_specs=(vmem,) * 3,
        scratch_shapes=held
        + [
            vm((rows, model), BF16),
            vm((GROUPS, rows, 2 * STATE), BF16),
            vm((n_tp - 1, rows, 2 * STATE), BF16),
            vm((width, rows * STATE), BF16),
            vm((width, LANES), F32),
            vm((rows, STATE), F32),
            vm((n_tp, rows, columns), BF16),
            vm((n_tp - 1, rows, columns), BF16),
            vm((2, n_z, n_ep, rows, columns), BF16),
            vm((n_ep, rows, LANES), F32),
            vm((n_ep * rows, 2 * experts * units), F32),
            vm((n_ep * rows, experts * units), BF16),
            vm((n_z, n_ep * rows, columns), BF16),
            vm((n_z, n_ep * rows, columns), BF16),
            vm((n_z, n_ep * rows, columns), F32),
            vm((n_z, n_ep, rows, columns), BF16),
            vm((n_same, rows, columns), BF16),
            dma((20,)),
            dma((7,)),
            dma((4,)),
            dma((n_z,)),
            dma((n_z,)),
            dma((2,)),
        ],
        compiler_params=pltpu.CompilerParams(
            collective_id=0,
            has_side_effects=True,
            vmem_limit_bytes=VMEM_LIMIT - 4 * rows * width * STATE - SPARE,
        ),
        name="layer",
    )(*operands)
    layer_out, new_state, new_filter = pl.pallas_call(
        finish_kernel,
        out_shape=outs,
        in_specs=[vmem] * 3,
        out_specs=(hbm,) * 3,
        scratch_shapes=[dma((3,))],
        compiler_params=pltpu.CompilerParams(vmem_limit_bytes=1024 * 1024),
        name="finish",
    )(layer_out, new_state, new_filter)
    return (
        layer_out,
        new_state.reshape(scan_state.shape),
        jnp.transpose(new_filter, (1, 0, 2)),
    )


def solution(mesh):
    in_specs = (
        P("ep", None),
        P("ep", None),
        P("ep", None),
        P(),
        P(None, "tp"),
        P(None, "tp"),
        P(None, "tp"),
        P("tp", None),
        P("tp", None),
        P("tp"),
        P("tp"),
        P("ep", "tp"),
        P(None, "tp"),
        P("ep", None, "tp"),
        P("ep", "tp", None, None),
        P("tp"),
        P("tp"),
        P("tp", None),
        P(),
        P("ep", None, "tp"),
        P("ep", None, "tp"),
        P("ep", "tp", None),
        P(None, "tp"),
        P(None, "tp"),
        P("tp", None),
    )
    out_specs = (P("ep", "tp"), P("ep", "tp", None, None), P("ep", None, "tp"))
    return jax.shard_map(
        on_device, mesh=mesh, in_specs=in_specs, out_specs=out_specs, check_vma=False
    )
```
